256 devices in a mesh: kv: 16 (over y, x), tp: 16 (over z, core).
Axes of the slice: x: 4, y: 4, z: 8, core: 2. Of those that a mesh axis runs over, the one named last changes fastest.
Arguments:
- tokens: bfloat16 [128, 4096], P(None, ('kv', 'tp')), may hold values from -41 to 41
- lengths: int32 [128], P('kv'), may hold values from 1 to 8192, 262144 in all
- retention_state: float32 [128, 16, 128, 256], P('kv', 'tp'), may hold values from -4 to 4
- mixer_gain: float32 [4096], P('kv'), may hold values from 0.1 to 1.9
- query_weight: bfloat16 [4096, 2048], P('kv', 'tp'), may hold values from -0.09375 to 0.09375
- key_weight: bfloat16 [4096, 2048], P('kv', 'tp'), may hold values from -0.09375 to 0.09375
- value_weight: bfloat16 [4096, 4096], P('kv', 'tp'), may hold values from -0.09375 to 0.09375
- gate_weight: bfloat16 [4096, 4096], P('kv', 'tp'), may hold values from -0.09375 to 0.09375
- output_weight: bfloat16 [4096, 4096], P('tp', 'kv'), may hold values from -0.125 to 0.125
- channel_gain: float32 [4096], P('kv'), may hold values from 0.1 to 1.9
- ffn_gate: bfloat16 [4096, 11264], P('kv', 'tp'), may hold values from -0.09375 to 0.09375
- ffn_up: bfloat16 [4096, 11264], P('kv', 'tp'), may hold values from -0.09375 to 0.09375
- ffn_down: bfloat16 [11264, 4096], P('tp', 'kv'), may hold values from -0.078125 to 0.078125
Outputs:
- layer_output: bfloat16 [128, 4096], P(None, ('kv', 'tp'))
- new_state: float32 [128, 16, 128, 256], P('kv', 'tp')
The draws below stay inside these ranges and needn't reach their ends.
All inputs are finite; a program needn't handle non-finite values. No bound on the sum of `lengths` on one device may be relied on, other than what follows from the above.
Results may differ from the reference program's by a relative error of at most 0.022.
Values may be sent and summed in bfloat16 or wider, within the bound.
A program may use at most 64 MiB of HBM per device.

```python
import math
import jax
import jax.numpy as jnp
import numpy as np
from jax import lax

BATCH = 128
D = 4096
HEADS = 16
QK = 128
VD = 256
FF = 11264
MAXLEN = 8192


def draw_tokens(key, part):
    subkeys = jax.random.split(key, 3)
    positions = jnp.arange(D, dtype=jnp.float32) / (D - 1)
    roughness = jnp.exp(jax.random.uniform(subkeys[0], (D,), minval=-0.3, maxval=0.3))
    column_scale = jnp.exp(jnp.log(0.3) + positions * jnp.log(10.0)) * roughness
    base_values = jnp.clip(jax.random.normal(subkeys[2], (BATCH, D)), -5.0, 5.0)
    row_scale = jnp.exp(jax.random.uniform(subkeys[1], (BATCH, 1), minval=jnp.log(0.5), maxval=jnp.log(2.0)))
    return (base_values * row_scale * column_scale[None, :]).astype(jnp.bfloat16)


def with_spikes(entries, stream_key, source, target, parts, factor):
    def block_of(position):
        return (jnp.arange(entries.shape[position]) // (entries.shape[position] // parts)).reshape((-1,) + (1,) * (entries.ndim - 1 - position))

    near = jax.random.permutation(stream_key, parts)[block_of(target)]
    other_side = (block_of(target) + parts // 2) % parts
    return jnp.where((block_of(source) == near) | (block_of(source) == other_side), factor * entries, entries)


def levels(own_key, extent, cuts, low, largest):
    level, own = 1.0, jax.random.fold_in(own_key, 6)
    for dim, shards_of in cuts:
        steps = jnp.exp(jax.random.uniform(jax.random.fold_in(own, dim), (shards_of,), jnp.float32, low / len(cuts), largest / len(cuts)))
        level = level * jnp.repeat(steps, extent[dim] // shards_of).reshape([-1 if axis == dim else 1 for axis in range(len(extent))])
    return level


def split_up(count, total, bound, skew):
    weights = [(1 << 20) // math.isqrt(grade ** skew) + 1 for grade in range(2, count + 1)]
    spare, holding = total - bound - (count - 1), [1] * (count - 1)
    while spare > 0:
        movable = [i for i in range(count - 1) if holding[i] < bound]
        mass, left = sum([weights[i] for i in movable]), spare
        for i in movable:
            more = min(bound - holding[i], max(1, left * weights[i] // mass), spare)
            holding[i] = holding[i] + more
            spare = spare - more
    return np.array([bound] + holding)


def uneven_parts(rng, number_of, total, limit, skew):
    if number_of == 2:
        one = jax.random.randint(rng, (), max(1, total - limit), min(limit, total - 1) + 1)
        return jnp.stack([one, total - one])
    tallies = jnp.asarray(split_up(number_of, total, limit, skew), jnp.int32)
    couples = (number_of - 1) // 2
    source_of, receiver = tallies[1:1 + 2 * couples:2], tallies[2:2 + 2 * couples:2]
    margin = jnp.minimum(source_of - 1, limit - receiver)
    moved = jax.random.randint(jax.random.fold_in(rng, 1), (couples,), 0, 1 << 20) % (margin + 1)
    tallies = tallies.at[1:1 + 2 * couples:2].set(source_of - moved).at[2:2 + 2 * couples:2].set(receiver + moved)
    return tallies[jax.random.permutation(jax.random.fold_in(rng, 2), number_of)]


def centred(rng, extent, width, bound, cuts=(), kind=jnp.bfloat16):
    values = jax.random.normal(rng, extent, jnp.float32) * width
    if len(cuts) > 0:
        values = levels(rng, extent, cuts, -0.22, 0.18) * values
    return jnp.clip(values, min=-bound, max=bound).astype(kind)


def bell_draw_with(stream_key, shape, spread, limit, cuts, heavy, kind=jnp.bfloat16):
    drawn = spread * jax.random.normal(stream_key, shape, jnp.float32)
    if cuts:
        drawn = drawn * levels(stream_key, shape, cuts, -0.22, 0.18)
    return jnp.clip(with_spikes(drawn, jax.random.fold_in(stream_key, 3), *heavy), -limit, limit).astype(kind)


def setup_inputs(seed: int = 0) -> dict:
    streams_of = jax.random.split(jax.random.key(seed), 14)
    return {
        "tokens": draw_tokens(jax.random.fold_in(streams_of[13], 71), 0),
        "lengths": uneven_parts(streams_of[1], BATCH, BATCH * MAXLEN // 4, MAXLEN, 2).astype(jnp.int32),
        "retention_state": centred(streams_of[2], (BATCH, HEADS, QK, VD), 0.3, 4.0, ((0, 16), (1, 16)), jnp.float32),
        "mixer_gain": jnp.clip(1.0 + 0.18 * jax.random.normal(streams_of[3], (D,), jnp.float32), 0.1, 1.9),
        "query_weight": centred(streams_of[4], (D, HEADS * QK), D ** -0.5, 0.09375, ((0, 16), (1, 16))),
        "key_weight": centred(streams_of[5], (D, HEADS * QK), D ** -0.5, 0.09375, ((0, 16), (1, 16))),
        "value_weight": centred(streams_of[6], (D, HEADS * VD), D ** -0.5, 0.09375, ((0, 16), (1, 16))),
        "gate_weight": centred(streams_of[7], (D, HEADS * VD), D ** -0.5, 0.09375, ((0, 16), (1, 16))),
        "output_weight": bell_draw_with(streams_of[8], (HEADS * VD, D), D ** -0.5, 0.125, ((0, 16), (1, 16)), (0, 1, 16, 2.0)),
        "channel_gain": jnp.clip(1.0 + 0.18 * jax.random.normal(streams_of[9], (D,), jnp.float32), 0.1, 1.9),
        "ffn_gate": centred(streams_of[10], (D, FF), D ** -0.5, 0.09375, ((0, 16), (1, 16))),
        "ffn_up": centred(streams_of[11], (D, FF), D ** -0.5, 0.09375, ((0, 16), (1, 16))),
        "ffn_down": bell_draw_with(streams_of[12], (FF, D), FF ** -0.5, 0.078125, ((0, 16), (1, 16)), (0, 1, 16, 2.0)),
    }


def rotate_heads(vectors, positions):
    half_dim = vectors.shape[-1] // 2
    frequency = 10000.0 ** (-jnp.arange(half_dim, dtype=jnp.float32) / half_dim)
    angles = positions.astype(jnp.float32)[:, None, None] * frequency
    cosine = jnp.cos(angles)
    sine_part = jnp.sin(angles)
    first_half = vectors[..., :half_dim]
    second = vectors[..., half_dim:]
    return jnp.concatenate([first_half * cosine - second * sine_part, first_half * sine_part + second * cosine], axis=-1)

def inverse_rms(values):
    return lax.rsqrt(lax.optimization_barrier(jnp.mean(values * values, axis=-1)) + 1e-06)

def reference(tokens, lengths, retention_state, mixer_gain, query_weight, key_weight, value_weight, gate_weight, output_weight, channel_gain, ffn_gate, ffn_up, ffn_down):
    batch_rows = tokens.shape[0]
    tokens_wide = tokens.astype(jnp.float32)
    scale_one = inverse_rms(tokens_wide)[:, None]
    normed = (tokens_wide * mixer_gain).astype(jnp.bfloat16)
    query_proj = jnp.dot(normed, query_weight, preferred_element_type=jnp.float32) * scale_one
    query_rows = rotate_heads(query_proj.reshape(batch_rows, HEADS, QK), lengths).astype(jnp.bfloat16)
    key_proj = jnp.dot(normed, key_weight, preferred_element_type=jnp.float32) * scale_one
    key_rows = (rotate_heads(key_proj.reshape(batch_rows, HEADS, QK), lengths) * QK ** (-0.5)).astype(jnp.bfloat16)
    value_rows = (jnp.dot(normed, value_weight, preferred_element_type=jnp.float32) * scale_one).astype(jnp.bfloat16)
    value_rows = value_rows.reshape(batch_rows, HEADS, VD)
    gate_rows = jnp.dot(normed, gate_weight, preferred_element_type=jnp.float32) * scale_one
    head_ids = jnp.arange(HEADS, dtype=jnp.float32)
    decay_rate = 1.0 - 2.0 ** (-5.0 - 10.0 * head_ids / (HEADS - 1))
    new_state = decay_rate[None, :, None, None] * retention_state + key_rows.astype(jnp.float32)[..., :, None] * value_rows.astype(jnp.float32)[..., None, :]
    retained = jnp.einsum('bhk,bhkv->bhv', query_rows.astype(jnp.float32), new_state, precision=lax.Precision.HIGHEST)
    normalized = retained * inverse_rms(retained)[..., None]
    merged = (normalized.reshape(batch_rows, HEADS * VD) * jax.nn.silu(gate_rows)).astype(jnp.bfloat16)
    residual = (tokens_wide + jnp.dot(merged, output_weight, preferred_element_type=jnp.float32)).astype(jnp.bfloat16)
    residual_wide = residual.astype(jnp.float32)
    scale_two = inverse_rms(residual_wide)[:, None]
    normed_two = (residual_wide * channel_gain).astype(jnp.bfloat16)
    gate_ff = jnp.dot(normed_two, ffn_gate, preferred_element_type=jnp.float32) * scale_two
    up_ff = jnp.dot(normed_two, ffn_up, preferred_element_type=jnp.float32) * scale_two
    hidden = (jax.nn.silu(gate_ff) * up_ff).astype(jnp.bfloat16)
    layer_output = (residual_wide + jnp.dot(hidden, ffn_down, preferred_element_type=jnp.float32)).astype(jnp.bfloat16)
    return (layer_output, new_state)
```

```python
import functools

import jax
import jax.numpy as jnp
from jax import lax
from jax.experimental import pallas as pl
from jax.experimental.pallas import tpu as pltpu
from jax.sharding import PartitionSpec as P

D = 4096
HEADS = 16
QK = 128
VD = 256
BATCH = 128
F32 = jnp.float32
BF16 = jnp.bfloat16


def ring_distance(offset, size):
    return min(offset, size - offset)


KV_OFFSETS = sorted(
    [(dy, dx) for dy in range(4) for dx in range(4) if (dy, dx) != (0, 0)],
    key=lambda o: -(ring_distance(o[0], 4) + ring_distance(o[1], 4)),
)
TP_OFFSETS = sorted(
    [(dz, dc) for dz in range(8) for dc in range(2) if (dz, dc) != (0, 0)],
    key=lambda o: -(2 * ring_distance(o[0], 8) + o[1]),
)
N_WEIGHT_COPIES = 12
(TOK, SQ1, QKVG, MERGED, MIXED, RESID, SQ2, FFN, HIDDEN, DOWN) = range(10)


def kernel(
    tokens_hbm,
    lengths,
    state_hbm,
    gain1_hbm,
    wq_hbm,
    wk_hbm,
    wv_hbm,
    wg_hbm,
    wo_hbm,
    gain2_hbm,
    fg_hbm,
    fu_hbm,
    fd_hbm,
    out_ref,
    new_state_hbm,
    tok_own,
    gain1,
    gain2,
    w_in,
    w_out,
    w_out_t,
    w_ff,
    w_down,
    w_down_t,
    state,
    new_state,
    tok_all,
    sq_own,
    sq_all,
    proj_own,
    proj_all,
    merged_own,
    merged_all,
    mixed_own,
    mixed_all,
    resid_own,
    resid_all,
    sq2_own,
    sq2_all,
    ffn_own,
    ffn_all,
    hidden_own,
    hidden_all,
    down_own,
    down_all,
    load_sem,
    store_sem,
    send_sem,
    recv_sem,
):
    kv = lax.axis_index("kv")
    tp = lax.axis_index("tp")
    ky, kx = kv // 4, kv % 4
    tz, tc = tp // 2, tp % 2
    kv_peers = [lax.rem(ky + dy, 4) * 4 + lax.rem(kx + dx, 4) for dy, dx in KV_OFFSETS]
    tp_peers = [
        lax.rem(tz + dz, 8) * 2 + (lax.rem(tc + dc, 2)) for dz, dc in TP_OFFSETS
    ]

    loads = {}
    for number, (name, source, target) in enumerate(
        [
            ("tok", tokens_hbm, tok_own),
            ("gain1", gain1_hbm, gain1),
            ("wq", wq_hbm, w_in.at[:, pl.ds(0, 128)]),
            ("wk", wk_hbm, w_in.at[:, pl.ds(128, 128)]),
            ("wv", wv_hbm, w_in.at[:, pl.ds(256, 256)]),
            ("wg", wg_hbm, w_in.at[:, pl.ds(512, 256)]),
            ("state", state_hbm, state),
            ("wo", wo_hbm, w_out),
            ("gain2", gain2_hbm, gain2),
            ("fg", fg_hbm, w_ff.at[pl.ds(0, 704), :]),
            ("fu", fu_hbm, w_ff.at[pl.ds(704, 704), :]),
            ("fd", fd_hbm, w_down),
        ]
    ):
        copy = pltpu.make_async_copy(source, target, load_sem.at[number])
        copy.start()
        loads[name] = copy

    barrier = pltpu.get_barrier_semaphore()
    for peer in tp_peers:
        pl.semaphore_signal(barrier, inc=1, device_id={"tp": peer}, device_id_type=pl.DeviceIdType.MESH)
    for peer in kv_peers:
        pl.semaphore_signal(barrier, inc=1, device_id={"kv": peer}, device_id_type=pl.DeviceIdType.MESH)

    def exchange(phase, axis, source_for, target):
        me, peers = (kv, kv_peers) if axis == "kv" else (tp, tp_peers)
        sends = []
        for peer in peers:
            copy = pltpu.make_async_remote_copy(
                src_ref=source_for(peer),
                dst_ref=target.at[me],
                send_sem=send_sem.at[phase, peer],
                recv_sem=recv_sem.at[phase, me],
                device_id={axis: peer},
                device_id_type=pl.DeviceIdType.MESH,
            )
            copy.start()
            sends.append(copy)

        def wait_recv():
            for peer in reversed(peers):
                pltpu.make_async_remote_copy(
                    src_ref=source_for(peer),
                    dst_ref=target.at[peer],
                    send_sem=send_sem.at[phase, peer],
                    recv_sem=recv_sem.at[phase, peer],
                    device_id={axis: peer},
                    device_id_type=pl.DeviceIdType.MESH,
                ).wait_recv()

        def wait_send():
            for copy in sends:
                copy.wait_send()

        pending.append(wait_send)
        return wait_recv

    pending = []

    lane = lax.broadcasted_iota(jnp.int32, (8, 128), 1) % 64
    row = lax.broadcasted_iota(jnp.int32, (8, 128), 0)
    frequency = jnp.ones((8, 128), F32)
    for bit in range(6):
        factor = 10000.0 ** (-(2.0**bit) / 64.0)
        frequency = jnp.where((lane // (2**bit)) % 2 == 1, frequency * factor, frequency)
    position = jnp.zeros((8, 128), F32)
    for r in range(8):
        position = jnp.where(row == r, lengths[r].astype(F32), position)
    angles = position * frequency
    cosine = jnp.cos(angles)
    sine = jnp.sin(angles)
    sine = jnp.where(lax.broadcasted_iota(jnp.int32, (8, 128), 1) < 64, -sine, sine)
    head = jnp.full((1, 256), tp, jnp.int32).astype(F32)
    decay = 1.0 - jnp.exp2(-5.0 - 10.0 * head / (HEADS - 1))

    loads["tok"].wait()
    pl.semaphore_wait(barrier, 30)

    wait_tokens = exchange(TOK, "tp", lambda peer: tok_own, tok_all)
    tok_all[tp] = tok_own[...]
    loads["gain1"].wait()
    for name in ("wq", "wk", "wv", "wg"):
        loads[name].wait()
    wait_tokens()

    def squares_and_normed(blocks, gain, own, everyone, phase):
        wide = blocks[...].reshape(256, BATCH).astype(F32)
        own[...] = jnp.sum(wide * wide, axis=0, keepdims=True)
        wait = exchange(phase, "kv", lambda peer: own, everyone)
        everyone[kv] = own[...]
        return (wide.T * gain[...]).astype(BF16), wait

    def inverse_rms(everyone):
        total = jnp.sum(everyone[...], axis=0)
        total = jnp.broadcast_to(total, (8, BATCH))
        mine = lax.broadcasted_iota(jnp.int32, (8, BATCH), 1) == (
            kv * 8 + lax.broadcasted_iota(jnp.int32, (8, BATCH), 0)
        )
        mean = jnp.sum(jnp.where(mine, total, 0.0), axis=1, keepdims=True) / D
        return lax.rsqrt(mean + 1e-06)

    normed, wait_squares = squares_and_normed(tok_all, gain1, sq_own, sq_all, SQ1)
    part = jnp.dot(normed, w_in[...], preferred_element_type=F32)
    proj_own[...] = part.reshape(16, 8, 768).astype(BF16)
    wait_proj = exchange(QKVG, "kv", lambda peer: proj_own.at[peer], proj_all)
    proj_all[kv] = proj_own[kv]

    loads["wo"].wait()
    w_out_t[...] = w_out[...].T
    loads["state"].wait()

    wait_squares()
    wait_proj()
    owned = jnp.sum(proj_all[...].astype(F32), axis=0) * inverse_rms(sq_all)

    def rotary(v):
        return v * cosine + pltpu.roll(v, 64, 1) * sine

    query = rotary(owned[:, :128]).astype(BF16).astype(F32)
    key = (rotary(owned[:, 128:256]) * QK ** (-0.5)).astype(BF16).astype(F32)
    value = owned[:, 256:512].astype(BF16).astype(F32)
    gate = owned[:, 512:768]

    query_t = query.T
    key_t = key.T
    crossed = jnp.sum(query * key, axis=1, keepdims=True)
    from_state = jnp.concatenate(
        [
            jnp.sum(query_t[:, s : s + 1] * state[s], axis=0, keepdims=True)
            for s in range(8)
        ],
        axis=0,
    )
    retained = decay * from_state + crossed * value
    normalized = retained * lax.rsqrt(
        jnp.mean(retained * retained, axis=1, keepdims=True) + 1e-06
    )
    merged_own[...] = (normalized * (gate / (1.0 + jnp.exp(-gate)))).astype(BF16)
    wait_merged = exchange(MERGED, "kv", lambda peer: merged_own, merged_all)
    merged_all[kv] = merged_own[...]

    for s in range(8):
        new_state[s] = decay * state[s] + key_t[:, s : s + 1] * value[s : s + 1, :]
    store_state = pltpu.make_async_copy(new_state, new_state_hbm, store_sem)
    store_state.start()

    wait_merged()

    def sums_over_tp(phase, weights_t, rows, own, everyone):
        part_t = lax.dot_general(
            weights_t, rows, (((1,), (1,)), ((), ())), preferred_element_type=F32
        )
        own[...] = part_t.reshape(16, 16, BATCH).astype(BF16)
        wait = exchange(phase, "tp", lambda peer: own.at[peer], everyone)
        everyone[tp] = own[tp]
        return wait

    rows = merged_all[...].astype(F32).reshape(BATCH, VD).astype(BF16)
    wait_mixed = sums_over_tp(MIXED, w_out_t[...], rows, mixed_own, mixed_all)
    loads["fd"].wait()
    w_down_t[:, pl.ds(640, 128)] = jnp.zeros((256, 128), BF16)
    w_down_t[:, pl.ds(0, 704)] = w_down[...].T
    loads["gain2"].wait()
    loads["fg"].wait()
    loads["fu"].wait()
    wait_mixed()
    mixed = jnp.sum(mixed_all[...].astype(F32), axis=0)
    resid_own[...] = (tok_own[...].astype(F32) + mixed).astype(BF16)
    wait_resid = exchange(RESID, "tp", lambda peer: resid_own, resid_all)
    resid_all[tp] = resid_own[...]
    wait_resid()

    normed2, wait_squares2 = squares_and_normed(resid_all, gain2, sq2_own, sq2_all, SQ2)
    part2 = lax.dot_general(
        normed2, w_ff[...], (((1,), (1,)), ((), ())), preferred_element_type=F32
    )
    ffn_own[...] = part2.reshape(16, 8, 1408).astype(BF16)
    wait_ffn = exchange(FFN, "kv", lambda peer: ffn_own.at[peer], ffn_all)
    ffn_all[kv] = ffn_own[kv]
    wait_squares2()
    wait_ffn()
    summed = jnp.sum(ffn_all[...].astype(F32), axis=0) * inverse_rms(sq2_all)
    gate_ff = summed[:, :704]
    up_ff = summed[:, 704:]
    hidden = gate_ff / (1.0 + jnp.exp(-gate_ff)) * up_ff
    hidden_own[...] = jnp.concatenate([hidden, jnp.zeros((8, 64), F32)], axis=1).astype(BF16)
    wait_hidden = exchange(HIDDEN, "kv", lambda peer: hidden_own, hidden_all)
    hidden_all[kv] = hidden_own[...]
    wait_hidden()

    rows2 = hidden_all[...].astype(F32).reshape(BATCH, 768).astype(BF16)
    wait_down = sums_over_tp(DOWN, w_down_t[...], rows2, down_own, down_all)
    for wait_send in pending[:-1]:
        wait_send()
    store_state.wait()
    wait_down()
    down = jnp.sum(down_all[...].astype(F32), axis=0)
    out_ref[...] = (resid_own[...].astype(F32) + down).astype(BF16)
    pending[-1]()


def on_device(
    tokens,
    lengths,
    retention_state,
    mixer_gain,
    query_weight,
    key_weight,
    value_weight,
    gate_weight,
    output_weight,
    channel_gain,
    ffn_gate,
    ffn_up,
    ffn_down,
):
    vmem = pltpu.VMEM
    out_t, new_state = pl.pallas_call(
        kernel,
        out_shape=(
            jax.ShapeDtypeStruct((16, BATCH), BF16),
            jax.ShapeDtypeStruct((8, QK, VD), F32),
        ),
        in_specs=[pl.BlockSpec(memory_space=pl.ANY)]
        + [pl.BlockSpec(memory_space=pltpu.SMEM)]
        + [pl.BlockSpec(memory_space=pl.ANY)] * 11,
        out_specs=(
            pl.BlockSpec(memory_space=vmem),
            pl.BlockSpec(memory_space=pl.ANY),
        ),
        scratch_shapes=[
            vmem((16, BATCH), BF16),
            vmem((1, 256), F32),
            vmem((1, 256), F32),
            vmem((256, 768), BF16),
            vmem((256, 256), BF16),
            vmem((256, 256), BF16),
            vmem((1408, 256), BF16),
            vmem((704, 256), BF16),
            vmem((256, 768), BF16),
            vmem((8, QK, VD), F32),
            vmem((8, QK, VD), F32),
            vmem((16, 16, BATCH), BF16),
            vmem((1, BATCH), F32),
            vmem((16, 1, BATCH), F32),
            vmem((16, 8, 768), BF16),
            vmem((16, 8, 768), BF16),
            vmem((8, VD), BF16),
            vmem((16, 8, VD), BF16),
            vmem((16, 16, BATCH), BF16),
            vmem((16, 16, BATCH), BF16),
            vmem((16, BATCH), BF16),
            vmem((16, 16, BATCH), BF16),
            vmem((1, BATCH), F32),
            vmem((16, 1, BATCH), F32),
            vmem((16, 8, 1408), BF16),
            vmem((16, 8, 1408), BF16),
            vmem((8, 768), BF16),
            vmem((16, 8, 768), BF16),
            vmem((16, 16, BATCH), BF16),
            vmem((16, 16, BATCH), BF16),
            pltpu.SemaphoreType.DMA((N_WEIGHT_COPIES,)),
            pltpu.SemaphoreType.DMA,
            pltpu.SemaphoreType.DMA((10, 16)),
            pltpu.SemaphoreType.DMA((10, 16)),
        ],
        compiler_params=pltpu.CompilerParams(
            collective_id=0, has_side_effects=True
        ),
    )(
        tokens.T,
        lengths,
        retention_state.reshape(8, QK, VD),
        mixer_gain.reshape(1, 256),
        query_weight,
        key_weight,
        value_weight,
        gate_weight,
        output_weight,
        channel_gain.reshape(1, 256),
        ffn_gate.T,
        ffn_up.T,
        ffn_down,
    )
    return out_t.T, new_state.reshape(8, 1, QK, VD)


def solution(mesh):
    in_specs = (
        P(None, ("kv", "tp")),
        P("kv"),
        P("kv", "tp", None, None),
        P("kv"),
        P("kv", "tp"),
        P("kv", "tp"),
        P("kv", "tp"),
        P("kv", "tp"),
        P("tp", "kv"),
        P("kv"),
        P("kv", "tp"),
        P("kv", "tp"),
        P("tp", "kv"),
    )
    out_specs = (P(None, ("kv", "tp")), P("kv", "tp", None, None))
    return jax.shard_map(
        on_device, mesh=mesh, in_specs=in_specs, out_specs=out_specs, check_vma=False
    )
```
